128 devices in a mesh: sp: 16 (over z, x), dp: 8 (over y, core).
Axes of the slice: x: 4, y: 4, z: 4, core: 2. Of those that a mesh axis runs over, the one named last changes fastest.
Arguments:
- activations: bfloat16 [8, 8192, 2048], P('dp', 'sp'), may hold values from -6 to 6
- value_weight: bfloat16 [2048, 1024], P(('sp', 'dp')), may hold values from -0.125 to 0.125
- gate_weight: bfloat16 [2048, 1024], P(('sp', 'dp')), may hold values from -0.125 to 0.125
- input_weight: bfloat16 [2048, 512], P(('sp', 'dp')), may hold values from -0.125 to 0.125
- readout_weight: bfloat16 [2048, 512], P(('sp', 'dp')), may hold values from -0.125 to 0.125
- rate_weight: bfloat16 [2048, 16], replicated, may hold values from -0.125 to 0.125
- value_taps: bfloat16 [4, 1024], replicated, may hold values from -0.375 to 0.375
- input_taps: bfloat16 [4, 512], replicated, may hold values from -3 to 3
- readout_taps: bfloat16 [4, 512], replicated, may hold values from -3 to 3
- rate_bias: float32 [16], replicated, may hold values from -1 to 1
- decay_log: float32 [16], replicated, may hold values from -1 to 1.5
- norm_gain: float32 [1024], replicated, may hold values from 0.1 to 1.9
- out_weight: bfloat16 [1024, 2048], P(None, ('sp', 'dp')), may hold values from -0.1875 to 0.1875
Outputs:
- mixed_out: bfloat16 [8, 8192, 2048], P('dp', 'sp')
The draws below stay inside these ranges and needn't reach their ends.
All inputs are finite; a program needn't handle non-finite values.
Results may differ from the reference program's by a relative error of at most 0.014.
Values may be sent and summed in bfloat16 or wider, within the bound.
A program may use at most 128 MiB of HBM per device.

```python
import jax
import jax.numpy as jnp
from jax import lax

D = 2048
HEADS = 16
HEAD_DIM = 64
GROUPS = 4
STATE = 128
CONV = 4
BLOCK = 64
WIDTH = 1024
LENGTH = 8192
SEQS = 8


def shard_levels(key, dims, shards, least, high):
    factor_of = 1.0
    for dim, blocks in shards:
        steps = jax.random.uniform(jax.random.fold_in(jax.random.fold_in(key, 6), dim), (blocks,), jnp.float32, least / len(shards), high / len(shards))
        factor_of = factor_of * jnp.repeat(jnp.exp(steps), dims[dim] // blocks).reshape((-1,) + (1,) * (len(dims) - 1 - dim))
    return factor_of


def normal_values(rng, shape, scale, reach, shards=(), kind=jnp.bfloat16):
    level = shard_levels(rng, shape, shards, -0.22, 0.18) if shards else 1.0
    entries = jax.random.normal(rng, shape, jnp.float32) * scale * level
    return jnp.minimum(jnp.maximum(entries, -reach), reach).astype(kind)


def setup_inputs(seed: int = 0) -> dict:
    streams_of = jax.random.split(jax.random.key(seed), 14)
    return {
        "activations": normal_values(streams_of[0], (SEQS, LENGTH, D), 1.0, 6.0, ((0, 8), (1, 16))),
        "value_weight": normal_values(streams_of[1], (D, WIDTH), D ** -0.5, 0.125, ((0, 128),)),
        "gate_weight": normal_values(streams_of[2], (D, WIDTH), D ** -0.5, 0.125, ((0, 128),)),
        "input_weight": normal_values(streams_of[3], (D, GROUPS * STATE), D ** -0.5, 0.125, ((0, 128),)),
        "readout_weight": normal_values(streams_of[4], (D, GROUPS * STATE), D ** -0.5, 0.125, ((0, 128),)),
        "rate_weight": normal_values(streams_of[5], (D, HEADS), D ** -0.5, 0.125),
        "value_taps": normal_values(streams_of[6], (CONV, WIDTH), (64 * CONV) ** -0.5, 0.375),
        "input_taps": normal_values(streams_of[7], (CONV, GROUPS * STATE), CONV ** -0.5, 3.0),
        "readout_taps": normal_values(streams_of[8], (CONV, GROUPS * STATE), CONV ** -0.5, 3.0),
        "rate_bias": jnp.clip(jax.random.uniform(streams_of[9], (HEADS,), jnp.float32, -1.0, 1.0), -1.0, 1.0),
        "decay_log": jnp.clip(jax.random.uniform(streams_of[10], (HEADS,), jnp.float32, -1.0, 1.5), -1.0, 1.5),
        "norm_gain": jnp.clip(1.0 + 0.18 * jax.random.normal(streams_of[11], (WIDTH,), jnp.float32), 0.1, 1.9),
        "out_weight": normal_values(streams_of[12], (WIDTH, D), WIDTH ** -0.5, 0.1875, ((1, 128),)),
    }


norm_eps = 1.0

def broaden(matrix, groups, head_count):
    row_count = matrix.shape[0]
    group_width = matrix.shape[1] // groups
    spread = matrix.reshape(row_count, groups, 1, group_width)
    spread = jnp.broadcast_to(spread, (row_count, groups, head_count // groups, group_width))
    return spread.reshape(row_count, head_count * group_width)

def causal_conv(series, kernel):
    extent = kernel.shape[0]
    length = series.shape[0]
    padded = jnp.pad(series.astype(jnp.float32), ((extent - 1, 0), (0, 0)))
    result = jnp.zeros(series.shape, jnp.float32)
    for offset in range(extent):
        result = result + kernel[offset].astype(jnp.float32) * padded[offset:offset + length]
    return result

def state_mix(values, inputs, readouts, rates, decay):
    length, head_count, head_width = values.shape
    blocks = length // BLOCK
    block_values = values.reshape(blocks, BLOCK, head_count, head_width).astype(jnp.float32)
    block_inputs = inputs.reshape(blocks, BLOCK, head_count, -1).astype(jnp.float32)
    block_reads = readouts.reshape(blocks, BLOCK, head_count, -1).astype(jnp.float32)
    block_rates = rates.reshape(blocks, BLOCK, head_count)
    running = jnp.cumsum(block_rates * decay, axis=1)
    by_head = jnp.transpose(running, (0, 2, 1))
    rate_head = jnp.transpose(block_rates, (0, 2, 1))
    causal = jnp.tril(jnp.ones((BLOCK, BLOCK), dtype=bool))
    intervals = by_head[:, :, :, None] - by_head[:, :, None, :]
    fading = jnp.where(causal, jnp.exp(jnp.minimum(intervals, 0.0)), 0.0)
    intersect = jnp.einsum('bthn,bshn->bhts', block_reads, block_inputs)
    scores = (intersect * fading * rate_head[:, :, None, :]).astype(jnp.bfloat16)
    within = jnp.einsum('bhts,bshp->bthp', scores.astype(jnp.float32), block_values)
    tail_fade = jnp.exp(running[:, -1:, :] - running) * block_rates
    weighted = (block_values * tail_fade[:, :, :, None]).astype(jnp.bfloat16)
    states = jnp.einsum('bshp,bshn->bhpn', weighted.astype(jnp.float32), block_inputs)
    totals = jnp.cumsum(running[:, -1, :], axis=0)
    starts = totals - running[:, -1, :]
    earlier = jnp.tril(jnp.ones((blocks, blocks), dtype=bool), -1)
    carried = jnp.where(earlier[:, :, None], jnp.exp(jnp.minimum(starts[:, None, :] - totals[None, :, :], 0.0)), 0.0)
    entering = jnp.einsum('cdh,dhpn->chpn', carried, states, precision=lax.Precision.HIGHEST)
    across = jnp.einsum('bthn,bhpn->bthp', block_reads, entering, precision=lax.Precision.HIGHEST)
    across = across * jnp.exp(running)[:, :, :, None]
    return (within + across).reshape(length, head_count * head_width)

def reference(activations, value_weight, gate_weight, input_weight, readout_weight, rate_weight, value_taps, input_taps, readout_taps, rate_bias, decay_log, norm_gain, out_weight):

    def mixer(sequence):
        length = sequence.shape[0]
        projected = jnp.dot(sequence, value_weight, preferred_element_type=jnp.float32).astype(jnp.bfloat16)
        gate_proj = jnp.dot(sequence, gate_weight, preferred_element_type=jnp.float32).astype(jnp.bfloat16)
        input_proj = jnp.dot(sequence, input_weight, preferred_element_type=jnp.float32).astype(jnp.bfloat16)
        readout_proj = jnp.dot(sequence, readout_weight, preferred_element_type=jnp.float32).astype(jnp.bfloat16)
        rate_raw = jnp.dot(sequence, rate_weight, preferred_element_type=jnp.float32).astype(jnp.bfloat16)
        conv_values = jax.nn.silu(causal_conv(projected, value_taps)).astype(jnp.bfloat16)
        conv_inputs = jax.nn.silu(causal_conv(input_proj, input_taps)).astype(jnp.bfloat16)
        conv_reads = jax.nn.silu(causal_conv(readout_proj, readout_taps)).astype(jnp.bfloat16)
        head_inputs = broaden(conv_inputs, GROUPS, HEADS).reshape(length, HEADS, STATE)
        head_reads = broaden(conv_reads, GROUPS, HEADS).reshape(length, HEADS, STATE)
        rates = jax.nn.softplus(rate_raw.astype(jnp.float32) + rate_bias)
        decay = -jnp.exp(decay_log) / length
        mixed = state_mix(conv_values.reshape(length, HEADS, HEAD_DIM), head_inputs, head_reads, rates, decay).astype(jnp.bfloat16)
        gated = mixed.astype(jnp.float32) * jax.nn.silu(gate_proj.astype(jnp.float32))
        scale = lax.rsqrt(lax.optimization_barrier(jnp.mean(gated * gated, axis=-1, keepdims=True)) + norm_eps)
        normed = (gated * scale * norm_gain).astype(jnp.bfloat16)
        return jnp.dot(normed, out_weight, preferred_element_type=jnp.float32).astype(jnp.bfloat16)
    return lax.map(mixer, activations)
```

```python
import jax
import jax.numpy as jnp
from jax import lax
from jax.experimental import pallas as pl
from jax.experimental.pallas import tpu as pltpu
from jax.sharding import PartitionSpec as P

F32 = jnp.float32
BF16 = jnp.bfloat16
MESH = pl.DeviceIdType.MESH

ROWS = 512
HALO = 16
LENGTH = 8192
WIDTH = 1024
BLOCK = 64
SPAN = 16

ORDER = (("x", "y", "z"), ("y", "z", "x"), ("z", "x", "y"))
STREAMS = ((0, 3), (3, 3), (6, 2))
VALUES, INPUTS, READS, GATE, OUT = (0, 3), 6, 1, (4, 7), (2, 5)


def silu(v):
    return (0.5 * v) * (1.0 + jnp.tanh(0.5 * v))


def rounded(v):
    return v.astype(BF16).astype(F32)


def split3(x):
    hi = x.astype(BF16)
    rest = x - hi.astype(F32)
    mid = rest.astype(BF16)
    return hi, mid, (rest - mid.astype(F32)).astype(BF16)


def dot(a, b):
    return jnp.dot(a, b, preferred_element_type=F32)


def spread(x, m):
    return sum(dot(part, m) for part in split3(x))


def kernel(
    act_hbm,
    wcat,
    rate_w,
    value_taps,
    input_taps,
    read_taps,
    bias,
    decay_log,
    gain,
    out,
    W,
    act,
    proj,
    rate_s,
    A,
    B,
    EM,
    VB,
    IT,
    R,
    SG,
    ST,
    EN,
    tb,
    tbuf,
    D,
    xs,
    rb,
    ps,
    pb,
    GT,
    NORM,
    ss,
    rs,
    ss2,
    rs2,
    ls,
):
    sp = lax.axis_index("sp")
    dp = lax.axis_index("dp")
    c = {"z": sp // 4, "x": sp % 4, "y": dp // 2}
    core = dp % 2
    other = 1 - core
    partner = (sp, c["y"] * 2 + other)

    def neighbour(d, step):
        at = dict(c)
        at[d] = (c[d] + step) % 4
        return at["z"] * 4 + at["x"], at["y"] * 2 + core

    load_act = pltpu.make_async_copy(act_hbm, act.at[pl.ds(HALO, ROWS)], ls.at[0])
    load_act.start()
    here = (c["z"], c["x"], c["y"])
    load_w = pltpu.make_async_copy(wcat.at[:, core], W.at[(slice(None), core, *here, core)], ls.at[1])
    load_w.start()

    barrier = pltpu.get_barrier_semaphore()

    def greet(d, carry):
        pl.semaphore_signal(barrier, inc=1, device_id=((sp + d) % SPAN, dp), device_id_type=MESH)
        return carry

    lax.fori_loop(1, SPAN, greet, 0)
    for peer in (neighbour("y", 1), neighbour("y", 3), partner):
        pl.semaphore_signal(barrier, inc=1, device_id=peer, device_id_type=MESH)
    pl.semaphore_wait(barrier, SPAN - 1 + 3)

    pending = []

    def copy(src, dst, k, device):
        return pltpu.make_async_remote_copy(
            src_ref=src,
            dst_ref=dst,
            send_sem=ss.at[k],
            recv_sem=rs.at[k],
            device_id=device,
            device_id_type=MESH,
        )

    def send(src, dst, k, device):
        started = copy(src, dst, k, device)
        started.start()
        pending.append(started)

    def arrived(dst, k):
        copy(dst, dst, k, partner).wait_recv()

    def piece(phase, color, first, count, index, half=None):
        dims = ORDER[color]
        at = dict(c)
        for d in dims[:phase]:
            at[d] = slice(None)
        at[dims[phase]] = index
        rows = slice(None)
        if half is not None:
            if phase == 0:
                rows = slice(half, half + 1)
            else:
                d = [d for d in "zxy" if d in dims[:phase]][0]
                at[d] = slice(2 * half, 2 * half + 2)
        return W.at[slice(first, first + count), core, at["z"], at["x"], at["y"], rows]

    def ring_start(phase, color, first, count, k):
        d = ORDER[color][phase]
        own = piece(phase, color, first, count, c[d])
        send(own, own, k, neighbour(d, 1))
        send(own, own, k + 1, neighbour(d, 3))

    def ring_pass(phase, color, first, count, k):
        d = ORDER[color][phase]
        for side, (back, ahead) in enumerate(((3, 1), (1, 3))):
            index = (c[d] + back) % 4
            arrived(piece(phase, color, first, count, index), k + side)
            half = piece(phase, color, first, count, index, side)
            send(half, half, k + 2 + side, neighbour(d, ahead))

    def ring_end(phase, color, first, count, k):
        index = (c[ORDER[color][phase]] + 2) % 4
        for side in range(2):
            arrived(piece(phase, color, first, count, index, side), k + 2 + side)

    def one(step, color):
        first, count = STREAMS[color]
        step(0, color, first, count, 4 * color)

    def two(step, stream):
        step(1, stream // 3, stream, 1, 12 + 4 * stream)

    def three(step, stream):
        step(2, stream // 3, stream, 1, 44 + 4 * stream)

    WAVES = ((0, 3, 6), (1, 4, 7), (2, 5))

    def share(stream):
        whole = W.at[stream, core]
        send(whole, whole, 76 + stream, partner)

    def shared(stream):
        arrived(W.at[stream, other], 76 + stream)

    SHARDS, EDGE = 84, 85

    def exchange_copy(q, src, dst, d):
        j = (sp + d) % SPAN
        return pltpu.make_async_remote_copy(
            src_ref=src(j),
            dst_ref=dst(sp),
            send_sem=ss2.at[q, d],
            recv_sem=rs2.at[q, sp],
            device_id=(j, dp),
            device_id_type=MESH,
        )

    def exchange_start(q, src, dst):
        def body(d, carry):
            exchange_copy(q, src, dst, d).start()
            return carry

        lax.fori_loop(1, SPAN, body, 0)

    def exchange_sent(q, src, dst):
        def body(d, carry):
            exchange_copy(q, src, dst, d).wait_send()
            return carry

        lax.fori_loop(1, SPAN, body, 0)

    def exchange_end(q, src, dst):
        def body(d, carry):
            i = (sp + d) % SPAN
            pltpu.make_async_remote_copy(
                src_ref=src(i),
                dst_ref=dst(i),
                send_sem=ss2.at[q, d],
                recv_sem=rs2.at[q, i],
                device_id=(i, dp),
                device_id_type=MESH,
            ).wait_recv()
            return carry

        lax.fori_loop(1, SPAN, body, 0)

    totals = (0, lambda j: tb, lambda i: tbuf.at[i])
    ends = (1, lambda j: xs.at[j // 2, j % 2], lambda i: rb.at[i])
    priors = (2, lambda j: ps.at[j], lambda i: pb.at[i // 2, i % 2])

    send(
        wcat.at[:, other], W.at[(slice(None), other, *here, core)], SHARDS, partner
    )
    send(
        act_hbm.at[pl.ds(ROWS - HALO, HALO)],
        act.at[pl.ds(0, HALO)],
        EDGE,
        ((sp + 1) % SPAN, dp),
    )
    load_w.wait()
    arrived(W.at[(slice(None), core, *here, other)], SHARDS)
    for color in range(3):
        one(ring_start, color)

    heads = lax.broadcasted_iota(jnp.int32, (16, WIDTH), 0)
    lanes = lax.broadcasted_iota(jnp.int32, (16, WIDTH), 1)
    expand = jnp.where(heads == lanes // 64, 1.0, 0.0).astype(BF16)
    load_act.wait()
    raw = rounded(dot(act[HALO : HALO + ROWS, :], rate_w[...])) + bias[...]
    rate_s[...] = jnp.maximum(raw, 0.0) + jnp.log1p(jnp.exp(-jnp.abs(raw)))

    for color in range(3):
        one(ring_pass, color)
    for color in range(3):
        one(ring_end, color)
    for stream in WAVES[0] + WAVES[1]:
        two(ring_start, stream)

    tri_r = lax.broadcasted_iota(jnp.int32, (BLOCK, BLOCK), 0)
    tri_c = lax.broadcasted_iota(jnp.int32, (BLOCK, BLOCK), 1)
    tri = jnp.where(tri_c <= tri_r, 1.0, 0.0).astype(BF16)
    decay = -jnp.exp(decay_log[...]) / LENGTH

    def fading(b, total):
        at = pl.ds(pl.multiple_of(b * BLOCK, BLOCK), BLOCK)
        rate = rate_s[at, :]
        running = sum(dot(tri, part) for part in split3(rate * decay))
        end = running[BLOCK - 1 : BLOCK, :]
        mid = 0.5 * end
        a = spread(jnp.exp(running - mid), expand)
        bb = spread(jnp.exp(mid - running) * rate, expand)
        for g in range(4):
            A[g, at, :] = a[:, g * 256 : g * 256 + 256]
            B[g, at, :] = bb[:, g * 256 : g * 256 + 256]
        EM[b] = spread(jnp.broadcast_to(jnp.exp(mid), (8, 16)), expand)
        return total + end

    total = lax.fori_loop(0, 4, fading, jnp.zeros((1, 16), F32))
    for stream in WAVES[0]:
        two(ring_pass, stream)
    total = lax.fori_loop(4, 8, fading, total)
    eye = jnp.where(
        lax.broadcasted_iota(jnp.int32, (16, 128), 0)
        == lax.broadcasted_iota(jnp.int32, (16, 128), 1),
        1.0,
        0.0,
    ).astype(BF16)
    tb[...] = spread(jnp.broadcast_to(total, (8, 16)), eye)
    tbuf[sp] = tb[...]
    for stream in WAVES[0]:
        two(ring_end, stream)
        three(ring_start, stream)
    for stream in WAVES[1]:
        two(ring_pass, stream)
    exchange_start(*totals)
    for stream in WAVES[1]:
        two(ring_end, stream)
    for stream in WAVES[2]:
        two(ring_start, stream)
    arrived(act.at[pl.ds(0, HALO)], EDGE)

    @pl.when(sp == 0)
    def _():
        act[0:HALO, :] = jnp.zeros((HALO, 2048), BF16)

    exchange_end(*totals)
    expand128 = jnp.where(
        lax.broadcasted_iota(jnp.int32, (128, WIDTH), 0)
        == lax.broadcasted_iota(jnp.int32, (128, WIDTH), 1) // 64,
        1.0,
        0.0,
    ).astype(BF16)
    factors = spread(jnp.exp(tbuf[...].reshape(128, 128)), expand128).reshape(SPAN, 8, WIDTH)
    D[0] = factors[:, :, :512]
    D[1] = factors[:, :, 512:]

    for stream in WAVES[0]:
        three(ring_pass, stream)
    for stream in WAVES[2]:
        two(ring_pass, stream)
    for stream in WAVES[1]:
        three(ring_start, stream)
    for stream in WAVES[2]:
        two(ring_end, stream)
    for stream in WAVES[0]:
        three(ring_end, stream)
        share(stream)

    def project(stream, cc):
        proj[...] = rounded(dot(act[...], W[stream, cc].reshape(2048, 256)))

    def convolved(at, taps):
        rows = proj[pl.ds(pl.multiple_of(at + 8, 8), 136), :]
        total = taps[3:4] * rows[8:136]
        for k in range(3):
            total = total + taps[k : k + 1] * rows[5 + k : 133 + k]
        return silu(total)

    def do_values(which, cc):
        g = 2 * which + cc
        project(VALUES[which], cc)
        taps = value_taps[:, g * 256 : g * 256 + 256].astype(F32)

        def body(i, carry):
            at = pl.multiple_of(i * 128, 128)
            v = rounded(convolved(at, taps))
            VB[g, pl.ds(at, 128), :] = (v * B[g, pl.ds(at, 128), :]).astype(BF16)
            return carry

        lax.fori_loop(0, 4, body, 0)

    def do_inputs(cc):
        project(INPUTS, cc)
        taps = input_taps[:, cc * 256 : cc * 256 + 256].astype(F32)

        def body(i, carry):
            at = pl.multiple_of(i * 128, 128)
            v = convolved(at, taps)
            for h in range(2):
                IT[2 * cc + h, :, pl.ds(at, 128)] = v[:, h * 128 : h * 128 + 128].T.astype(BF16)
            return carry

        lax.fori_loop(0, 4, body, 0)

    def do_reads(cc):
        project(READS, cc)
        taps = read_taps[:, cc * 256 : cc * 256 + 256].astype(F32)

        def body(i, carry):
            at = pl.multiple_of(i * 128, 128)
            v = convolved(at, taps).astype(BF16)
            for h in range(2):
                R[2 * cc + h, pl.ds(at, 128), :] = v[:, h * 128 : h * 128 + 128]
            return carry

        lax.fori_loop(0, 4, body, 0)

    def do_gate(which, cc):
        g = 2 * which + cc
        project(GATE[which], cc)

        def body(i, carry):
            at = pl.multiple_of(i * 128, 128)
            SG[g, pl.ds(at, 128), :] = silu(proj[pl.ds(at + HALO, 128), :])
            return carry

        lax.fori_loop(0, 4, body, 0)

    for stream in WAVES[0]:
        shared(stream)
    do_inputs(0)
    do_inputs(1)
    do_values(0, 0)
    for stream in WAVES[1]:
        three(ring_pass, stream)
    for stream in WAVES[2]:
        three(ring_start, stream)
    do_values(0, 1)
    do_values(1, 0)
    do_values(1, 1)

    def block_states(i, carry):
        at = pl.ds(pl.multiple_of(i * 128, 128), 128)
        zero = jnp.zeros((BLOCK, 256), BF16)
        for g in range(4):
            v = VB[g, at, :]
            both = jnp.concatenate(
                [
                    jnp.concatenate([v[:BLOCK], zero], axis=0),
                    jnp.concatenate([zero, v[BLOCK:]], axis=0),
                ],
                axis=1,
            )
            states = dot(IT[g, :, at], both)
            ST[g, 2 * i] = states[:, :256]
            ST[g, 2 * i + 1] = states[:, 256:]
        return carry

    lax.fori_loop(0, 4, block_states, 0)
    for stream in WAVES[1]:
        three(ring_end, stream)
        share(stream)
    for g in range(4):
        x = jnp.zeros((128, 256), F32)
        for b in range(8):
            em = EM[b, 0:1, g * 256 : g * 256 + 256]
            x = em * (em * x + ST[g, b])
        for n in range(8):
            xs[n, g // 2, :, (g % 2) * 256 : (g % 2) * 256 + 256] = x[n * 16 : n * 16 + 16].astype(
                BF16
            )
    exchange_start(*ends)
    keep = pltpu.make_async_copy(xs.at[sp // 2, sp % 2], rb.at[sp], ls.at[2])
    keep.start()
    for stream in WAVES[1]:
        shared(stream)
    do_reads(0)
    do_reads(1)
    for stream in WAVES[2]:
        three(ring_pass, stream)
    keep.wait()
    exchange_end(*ends)

    half = sp % 2

    def prefix(i, x):
        ps[i] = x.astype(BF16)
        return D[half, i][0:1, :] * x + rb[i].astype(F32)

    lax.fori_loop(0, SPAN, prefix, jnp.zeros((16, 512), F32))
    exchange_start(*priors)
    keep = pltpu.make_async_copy(ps.at[sp], pb.at[sp // 2, sp % 2], ls.at[2])
    keep.start()
    do_gate(0, 0)
    do_gate(0, 1)
    for stream in WAVES[2]:
        three(ring_end, stream)
        share(stream)
    do_gate(1, 0)
    do_gate(1, 1)
    keep.wait()
    exchange_end(*priors)
    for g in range(4):
        lane = (g % 2) * 256
        x = pb[:, g // 2, :, lane : lane + 256].reshape(128, 256).astype(F32)
        for b in range(8):
            em = EM[b, 0:1, g * 256 : g * 256 + 256]
            EN[g, b] = (em * x).astype(BF16)
            x = em * (em * x + ST[g, b])

    row = lax.broadcasted_iota(jnp.int32, (128, 128), 0)
    col = lax.broadcasted_iota(jnp.int32, (128, 128), 1)
    causal = (col <= row) & (row // BLOCK == col // BLOCK)

    def finish(i, carry):
        at = pl.ds(pl.multiple_of(i * 128, 128), 128)
        squares = jnp.zeros((128, 1), F32)
        for g in range(4):
            r = R[g, at, :]
            scores = jnp.where(causal, dot(r, IT[g, :, at]), 0.0).astype(BF16)
            across = jnp.concatenate(
                [dot(r[:BLOCK], EN[g, 2 * i]), dot(r[BLOCK:], EN[g, 2 * i + 1])], axis=0
            )
            mixed = A[g, at, :] * (dot(scores, VB[g, at, :]) + across)
            gated = rounded(mixed) * SG[g, at, :]
            GT[g] = gated
            squares = squares + jnp.sum(gated * gated, axis=1, keepdims=True)
        scale = lax.rsqrt(squares / WIDTH + 1.0)
        for g in range(4):
            lane = g * 256
            NORM[at, lane : lane + 256] = (GT[g] * scale * gain[:, lane : lane + 256]).astype(BF16)
        return carry

    lax.fori_loop(0, 4, finish, 0)
    for stream in WAVES[2]:
        shared(stream)

    def project_out(n, carry):
        w = jnp.concatenate(
            [
                W[OUT[q // 2], q % 2, n // 2, pl.ds((n % 2) * 2, 2)].reshape(256, 256)
                for q in range(4)
            ],
            axis=1,
        )
        tile = lax.dot_general(
            NORM[...], w, (((1,), (1,)), ((), ())), preferred_element_type=F32
        )
        out[:, pl.ds(pl.multiple_of(n * 256, 256), 256)] = tile.astype(BF16)
        return carry

    lax.fori_loop(0, 8, project_out, 0)

    for started in pending:
        started.wait_send()
    for q in (totals, ends, priors):
        exchange_sent(*q)


def per_device(
    activations,
    value_weight,
    gate_weight,
    input_weight,
    readout_weight,
    rate_weight,
    value_taps,
    input_taps,
    readout_taps,
    rate_bias,
    decay_log,
    norm_gain,
    out_weight,
):
    out_rows = out_weight.T
    streams = jnp.concatenate(
        [
            value_weight[:, :512],
            readout_weight,
            out_rows[:, :512],
            value_weight[:, 512:],
            gate_weight[:, :512],
            out_rows[:, 512:],
            input_weight,
            gate_weight[:, 512:],
        ],
        axis=1,
    )
    wcat = jnp.transpose(streams.reshape(16, 8, 2, 256), (1, 2, 0, 3))
    vmem = pl.BlockSpec(memory_space=pltpu.VMEM)
    result = pl.pallas_call(
        kernel,
        out_shape=jax.ShapeDtypeStruct((ROWS, 2048), BF16),
        in_specs=[pl.BlockSpec(memory_space=pl.ANY)] + [vmem] * 8,
        out_specs=vmem,
        scratch_shapes=[
            pltpu.VMEM((8, 2, 4, 4, 4, 2, 16, 256), BF16),
            pltpu.VMEM((HALO + ROWS, 2048), BF16),
            pltpu.VMEM((HALO + ROWS, 256), F32),
            pltpu.VMEM((ROWS, 16), F32),
            pltpu.VMEM((4, ROWS, 256), F32),
            pltpu.VMEM((4, ROWS, 256), F32),
            pltpu.VMEM((8, 8, WIDTH), F32),
            pltpu.VMEM((4, ROWS, 256), BF16),
            pltpu.VMEM((4, 128, ROWS), BF16),
            pltpu.VMEM((4, ROWS, 128), BF16),
            pltpu.VMEM((4, ROWS, 256), F32),
            pltpu.VMEM((4, 8, 128, 256), F32),
            pltpu.VMEM((4, 8, 128, 256), BF16),
            pltpu.VMEM((8, 128), F32),
            pltpu.VMEM((SPAN, 8, 128), F32),
            pltpu.VMEM((2, SPAN, 8, 512), F32),
            pltpu.VMEM((8, 2, 16, 512), BF16),
            pltpu.VMEM((SPAN, 16, 512), BF16),
            pltpu.VMEM((SPAN, 16, 512), BF16),
            pltpu.VMEM((8, 2, 16, 512), BF16),
            pltpu.VMEM((4, 128, 256), F32),
            pltpu.VMEM((ROWS, WIDTH), BF16),
            pltpu.SemaphoreType.DMA((86,)),
            pltpu.SemaphoreType.DMA((86,)),
            pltpu.SemaphoreType.DMA((3, SPAN)),
            pltpu.SemaphoreType.DMA((3, SPAN)),
            pltpu.SemaphoreType.DMA((3,)),
        ],
        compiler_params=pltpu.CompilerParams(
            collective_id=0, has_side_effects=True, vmem_limit_bytes=60 * 2**20
        ),
        name="mixer",
    )(
        activations[0],
        wcat,
        rate_weight,
        value_taps,
        input_taps,
        readout_taps,
        rate_bias[None],
        decay_log[None],
        norm_gain[None],
    )
    return result[None]


def solution(mesh):
    placed = (
        P("dp", "sp", None),
        P(("sp", "dp"), None),
        P(("sp", "dp"), None),
        P(("sp", "dp"), None),
        P(("sp", "dp"), None),
        P(),
        P(),
        P(),
        P(),
        P(),
        P(),
        P(),
        P(None, ("sp", "dp")),
    )
    return jax.shard_map(
        per_device, mesh=mesh, in_specs=placed, out_specs=P("dp", "sp", None), check_vma=False
    )
```

```python
import jax
import jax.numpy as jnp
from jax import lax
from jax.experimental import pallas as pl
from jax.experimental.pallas import tpu as pltpu
from jax.sharding import PartitionSpec as P

F32 = jnp.float32
BF16 = jnp.bfloat16
MESH = pl.DeviceIdType.MESH

ROWS = 512
HALO = 16
LENGTH = 8192
WIDTH = 1024
BLOCK = 64
SPAN = 16

ORDER = (("x", "y", "z"), ("z", "x", "y"), ("y", "z", "x"))
STREAMS = ((0, 3), (3, 3), (6, 2))
VALUES, INPUTS, READS, GATE, OUT = (0, 3), 6, 1, (4, 7), (2, 5)


def silu(v):
    return (0.5 * v) * (1.0 + jnp.tanh(0.5 * v))


def rounded(v):
    return v.astype(BF16).astype(F32)


def split3(x):
    hi = x.astype(BF16)
    rest = x - hi.astype(F32)
    mid = rest.astype(BF16)
    return hi, mid, (rest - mid.astype(F32)).astype(BF16)


def dot(a, b):
    return jnp.dot(a, b, preferred_element_type=F32)


def spread(x, m):
    return sum(dot(part, m) for part in split3(x))


def kernel(
    act_hbm,
    value_w,
    gate_w,
    input_w,
    read_w,
    out_w,
    rate_w,
    value_taps,
    input_taps,
    read_taps,
    bias,
    decay_log,
    gain,
    out,
    W,
    wcat,
    act,
    proj,
    rate_s,
    A,
    B,
    EM,
    VB,
    IT,
    R,
    SG,
    ST,
    EN,
    tb,
    tbuf,
    D,
    xs,
    rb,
    ps,
    pb,
    GT,
    NORM,
    ss,
    rs,
    ss2,
    rs2,
    ls,
    gs,
):
    sp = lax.axis_index("sp")
    dp = lax.axis_index("dp")
    c = {"z": sp // 4, "x": sp % 4, "y": dp // 2}
    core = dp % 2
    other = 1 - core
    partner = (sp, c["y"] * 2 + other)

    def neighbour(d, step, side=None):
        at = dict(c)
        at[d] = (c[d] + step) % 4
        return at["z"] * 4 + at["x"], at["y"] * 2 + (core if side is None else side)

    load_act = pltpu.make_async_copy(act_hbm, act.at[pl.ds(HALO, ROWS)], ls.at[0])
    load_act.start()
    here = (c["z"], c["x"], c["y"])
    shards = (
        (value_w, 0),
        (read_w, 0),
        (out_w, 0),
        (value_w, 512),
        (gate_w, 0),
        (out_w, 512),
        (input_w, 0),
        (gate_w, 512),
    )

    load_w = [
        pltpu.make_async_copy(ref.at[:, pl.ds(at, 512)], wcat.at[stream], ls.at[3 + stream])
        for stream, (ref, at) in enumerate(shards)
    ]
    for load in load_w:
        load.start()

    barrier = pltpu.get_barrier_semaphore()

    lines = [
        neighbour(d, step, side) for d in "xyz" for step in (1, 2, 3) for side in (core, other)
    ]
    for peer in lines + [partner]:
        pl.semaphore_signal(barrier, inc=1, device_id=peer, device_id_type=MESH)
    for load in load_w:
        load.wait()
    pl.semaphore_wait(barrier, 19)
    for step in (1, 2, 3):
        pl.semaphore_signal(gs, inc=1, device_id=neighbour("x", step), device_id_type=MESH)

    pending = []

    def copy(src, dst, sent, landed, device):
        return pltpu.make_async_remote_copy(
            src_ref=src,
            dst_ref=dst,
            send_sem=ss.at[sent],
            recv_sem=rs.at[landed],
            device_id=device,
            device_id_type=MESH,
        )

    def send(src, dst, k, device, landed=None):
        started = copy(src, dst, k, k if landed is None else landed, device)
        started.start()
        pending.append(started)

    def arrived(dst, k):
        copy(dst, dst, k, k, partner).wait_recv()

    def line_start(color):
        first, count = STREAMS[color]
        for t, step in enumerate((1, 3, 2)):
            for side in range(2):
                send(
                    wcat.at[first : first + count, :, side * 256 : side * 256 + 256],
                    W.at[(slice(first, first + count), side, *here, core)],
                    (color * 3 + t) * 2 + side,
                    neighbour(ORDER[color][0], step, side),
                    (color * 3 + t) * 2 + core,
                )

    def line_end(color):
        first, count = STREAMS[color]
        for t, step in enumerate((1, 3, 2)):
            at = dict(c)
            at[ORDER[color][0]] = (at[ORDER[color][0]] - step) % 4
            for side in range(2):
                arrived(
                    W.at[first : first + count, core, at["z"], at["x"], at["y"], side],
                    (color * 3 + t) * 2 + side,
                )

    def piece(phase, stream, index, half=None, side=None):
        dims = ORDER[stream // 3]
        at = dict(c)
        for d in dims[:phase]:
            at[d] = slice(None)
        at[dims[phase]] = index
        if half is not None:
            d = [d for d in "zxy" if d in dims[:phase]][0]
            at[d] = slice(2 * half, 2 * half + 2)
        return W.at[stream, core if side is None else side, at["z"], at["x"], at["y"]]

    def axis(phase, stream):
        d = ORDER[stream // 3][phase]
        return d, c[d], 18 + 48 * (phase - 1) + 6 * stream

    def ring_start(phase, stream, parts=(0, 1)):
        d, i, k = axis(phase, stream)
        halves = [piece(phase, stream, i, half) for half in range(2)]
        for j in parts:
            send(halves[j], halves[j], k + j, neighbour(d, 1))
            send(halves[1 - j], halves[1 - j], k + 2 + j, neighbour(d, 3))

    def ring_pass(phase, stream):
        d, i, k = axis(phase, stream)
        for side, (back, ahead) in enumerate(((3, 1), (1, 3))):
            half = piece(phase, stream, (i + back) % 4, side)
            arrived(half, k + 2 * side)
            send(half, half, k + 4 + side, neighbour(d, ahead))

    def ring_rest(phase, stream):
        d, i, k = axis(phase, stream)
        arrived(piece(phase, stream, (i + 3) % 4, 1), k + 1)
        arrived(piece(phase, stream, (i + 1) % 4, 0), k + 3)

    def ring_end(phase, stream):
        d, i, k = axis(phase, stream)
        for side in range(2):
            arrived(piece(phase, stream, (i + 2) % 4, side), k + 4 + side)

    def share(stream, step):
        i = (axis(2, stream)[1] + step) % 4
        plane = piece(2, stream, i)
        send(plane, plane, 114 + 4 * stream + step, partner)

    def shared(stream):
        for step in range(4):
            i = (axis(2, stream)[1] + step) % 4
            arrived(piece(2, stream, i, None, other), 114 + 4 * stream + step)

    def planes_start(streams):
        for stream in streams:
            ring_start(1, stream)

    def planes_pass(streams):
        for stream in streams:
            ring_pass(1, stream)

    def planes_end(streams):
        for stream in streams:
            ring_rest(1, stream)
            ring_end(1, stream)

    def cube_start(streams, parts=(0, 1)):
        for j in parts:
            for stream in streams:
                ring_start(2, stream, (j,))
                if j == 0:
                    share(stream, 0)

    def cube_pass(streams):
        for stream in streams:
            ring_pass(2, stream)

    def cube_rest(streams):
        for stream in streams:
            ring_rest(2, stream)
            share(stream, 1)
            share(stream, 3)

    def cube_end(streams):
        for stream in streams:
            ring_end(2, stream)
            share(stream, 2)

    def cube_shared(streams):
        for stream in streams:
            shared(stream)

    WAVES = ((6, 0, 3), (1, 4, 7), (2, 5))
    EDGE, GIVEN = 146, 147

    def exchange_copy(q, src, dst, d):
        j = (sp + d) % SPAN
        return pltpu.make_async_remote_copy(
            src_ref=src(j),
            dst_ref=dst(sp),
            send_sem=ss2.at[q, d],
            recv_sem=rs2.at[q, sp],
            device_id=(j, dp),
            device_id_type=MESH,
        )

    def exchange_start(q, src, dst):
        def body(d, carry):
            exchange_copy(q, src, dst, d).start()
            return carry

        lax.fori_loop(1, SPAN, body, 0)

    def exchange_sent(q, src, dst):
        def body(d, carry):
            exchange_copy(q, src, dst, d).wait_send()
            return carry

        lax.fori_loop(1, SPAN, body, 0)

    def exchange_end(q, src, dst):
        def body(d, carry):
            i = (sp + d) % SPAN
            pltpu.make_async_remote_copy(
                src_ref=src(i),
                dst_ref=dst(i),
                send_sem=ss2.at[q, d],
                recv_sem=rs2.at[q, i],
                device_id=(i, dp),
                device_id_type=MESH,
            ).wait_recv()
            return carry

        lax.fori_loop(1, SPAN, body, 0)

    totals = (0, lambda j: tb, lambda i: tbuf.at[i])
    ends = (1, lambda j: xs.at[j // 2, j % 2], lambda i: rb.at[i])
    priors = (2, lambda j: ps.at[j], lambda i: pb.at[i // 2, i % 2])

    for color in range(3):
        line_start(color)
    send(
        wcat.at[:, :, pl.ds(pl.multiple_of(other * 256, 256), 256)],
        W.at[(slice(None), other, *here, core)],
        GIVEN,
        partner,
    )
    keep_w = pltpu.make_async_copy(
        wcat.at[:, :, pl.ds(pl.multiple_of(core * 256, 256), 256)],
        W.at[(slice(None), core, *here, core)],
        ls.at[1],
    )
    keep_w.start()
    keep_w.wait()
    arrived(W.at[(slice(None), core, *here, other)], GIVEN)
    for color in range(3):
        line_end(color)
    planes_start(WAVES[0])
    planes_start(WAVES[1])
    pl.semaphore_wait(gs, 3)
    send(
        act_hbm.at[pl.ds(ROWS - HALO, HALO)],
        act.at[pl.ds(0, HALO)],
        EDGE,
        ((sp + 1) % SPAN, dp),
    )

    heads = lax.broadcasted_iota(jnp.int32, (16, WIDTH), 0)
    lanes = lax.broadcasted_iota(jnp.int32, (16, WIDTH), 1)
    expand = jnp.where(heads == lanes // 64, 1.0, 0.0).astype(BF16)
    load_act.wait()
    raw = lax.dot_general(
        act[HALO : HALO + ROWS, :],
        rate_w[...],
        (((1,), (1,)), ((), ())),
        preferred_element_type=F32,
    )
    raw = rounded(raw) + bias[...]
    rate_s[...] = jnp.maximum(raw, 0.0) + jnp.log1p(jnp.exp(-jnp.abs(raw)))

    tri_r = lax.broadcasted_iota(jnp.int32, (BLOCK, BLOCK), 0)
    tri_c = lax.broadcasted_iota(jnp.int32, (BLOCK, BLOCK), 1)
    tri = jnp.where(tri_c <= tri_r, 1.0, 0.0).astype(BF16)
    decay = -jnp.exp(decay_log[...]) / LENGTH

    def fading(b, total):
        at = pl.ds(pl.multiple_of(b * BLOCK, BLOCK), BLOCK)
        rate = rate_s[at, :]
        running = sum(dot(tri, part) for part in split3(rate * decay))
        end = running[BLOCK - 1 : BLOCK, :]
        mid = 0.5 * end
        a = spread(jnp.exp(running - mid), expand)
        bb = spread(jnp.exp(mid - running) * rate, expand)
        for g in range(4):
            A[g, at, :] = a[:, g * 256 : g * 256 + 256]
            B[g, at, :] = bb[:, g * 256 : g * 256 + 256]
        EM[b] = spread(jnp.broadcast_to(jnp.exp(mid), (8, 16)), expand)
        return total + end

    planes_pass(WAVES[0])
    total = lax.fori_loop(0, 3, fading, jnp.zeros((1, 16), F32))
    planes_end(WAVES[0])
    cube_start(WAVES[0])
    planes_pass(WAVES[1])
    total = lax.fori_loop(3, 6, fading, total)
    planes_start(WAVES[2])
    total = lax.fori_loop(6, 8, fading, total)
    eye = jnp.where(
        lax.broadcasted_iota(jnp.int32, (16, 128), 0)
        == lax.broadcasted_iota(jnp.int32, (16, 128), 1),
        1.0,
        0.0,
    ).astype(BF16)
    tb[...] = spread(jnp.broadcast_to(total, (8, 16)), eye)
    tbuf[sp] = tb[...]
    exchange_start(*totals)
    cube_pass(WAVES[0])
    planes_end(WAVES[1])
    cube_start(WAVES[1])
    planes_pass(WAVES[2])
    arrived(act.at[pl.ds(0, HALO)], EDGE)

    @pl.when(sp == 0)
    def _():
        act[0:HALO, :] = jnp.zeros((HALO, 2048), BF16)

    exchange_end(*totals)
    expand128 = jnp.where(
        lax.broadcasted_iota(jnp.int32, (128, WIDTH), 0)
        == lax.broadcasted_iota(jnp.int32, (128, WIDTH), 1) // 64,
        1.0,
        0.0,
    ).astype(BF16)
    factors = spread(jnp.exp(tbuf[...].reshape(128, 128)), expand128).reshape(SPAN, 8, WIDTH)
    D[0] = factors[:, :, :512]
    D[1] = factors[:, :, 512:]

    cube_rest(WAVES[0])
    planes_end(WAVES[2])
    cube_end(WAVES[0])

    def project(stream):
        w = jnp.concatenate([W[stream, cc].reshape(2048, 256) for cc in range(2)], axis=1)
        proj[...] = rounded(dot(act[...], w))

    def convolved(at, lane, taps):
        rows = proj[pl.ds(pl.multiple_of(at + 8, 8), 136), lane : lane + 256]
        total = taps[3:4] * rows[8:136]
        for k in range(3):
            total = total + taps[k : k + 1] * rows[5 + k : 133 + k]
        return silu(total)

    def over_rows(body):
        def step(i, carry):
            body(pl.multiple_of(i * 128, 128))
            return carry

        lax.fori_loop(0, 4, step, 0)

    def do_values(which):
        lane = which * 512
        taps = value_taps[:, lane : lane + 512].astype(F32)

        def body(at):
            for cc in range(2):
                v = rounded(convolved(at, cc * 256, taps[:, cc * 256 : cc * 256 + 256]))
                g = 2 * which + cc
                VB[g, pl.ds(at, 128), :] = (v * B[g, pl.ds(at, 128), :]).astype(BF16)

        over_rows(body)

    def do_inputs():
        taps = input_taps[...].astype(F32)

        def body(at):
            for cc in range(2):
                v = convolved(at, cc * 256, taps[:, cc * 256 : cc * 256 + 256])
                for h in range(2):
                    part = v[:, h * 128 : h * 128 + 128]
                    IT[2 * cc + h, :, pl.ds(at, 128)] = part.T.astype(BF16)

        over_rows(body)

    def do_reads():
        taps = read_taps[...].astype(F32)

        def body(at):
            for cc in range(2):
                v = convolved(at, cc * 256, taps[:, cc * 256 : cc * 256 + 256]).astype(BF16)
                for h in range(2):
                    R[2 * cc + h, pl.ds(at, 128), :] = v[:, h * 128 : h * 128 + 128]

        over_rows(body)

    def do_gate(which):
        def body(at):
            for cc in range(2):
                SG[2 * which + cc, pl.ds(at, 128), :] = silu(
                    proj[pl.ds(at + HALO, 128), cc * 256 : cc * 256 + 256]
                )

        over_rows(body)

    shared(INPUTS)
    project(INPUTS)
    cube_pass(WAVES[1])
    do_inputs()
    shared(VALUES[0])
    project(VALUES[0])
    do_values(0)
    cube_start(WAVES[2], (0,))
    cube_rest(WAVES[1])
    shared(VALUES[1])
    project(VALUES[1])
    do_values(1)

    def block_states(i, carry):
        at = pl.ds(pl.multiple_of(i * 128, 128), 128)
        zero = jnp.zeros((BLOCK, 256), BF16)
        for g in range(4):
            v = VB[g, at, :]
            both = jnp.concatenate(
                [
                    jnp.concatenate([v[:BLOCK], zero], axis=0),
                    jnp.concatenate([zero, v[BLOCK:]], axis=0),
                ],
                axis=1,
            )
            states = dot(IT[g, :, at], both)
            ST[g, 2 * i] = states[:, :256]
            ST[g, 2 * i + 1] = states[:, 256:]
        return carry

    lax.fori_loop(0, 4, block_states, 0)
    for g in range(4):
        x = jnp.zeros((128, 256), F32)
        for b in range(8):
            em = EM[b, 0:1, g * 256 : g * 256 + 256]
            x = em * (em * x + ST[g, b])
        for n in range(8):
            xs[n, g // 2, :, (g % 2) * 256 : (g % 2) * 256 + 256] = x[n * 16 : n * 16 + 16].astype(
                BF16
            )
    exchange_start(*ends)
    keep = pltpu.make_async_copy(xs.at[sp // 2, sp % 2], rb.at[sp], ls.at[2])
    keep.start()
    cube_start(WAVES[2], (1,))
    cube_end(WAVES[1])
    shared(READS)
    project(READS)
    cube_pass(WAVES[2])
    do_reads()
    shared(GATE[0])
    project(GATE[0])
    do_gate(0)
    cube_rest(WAVES[2])
    keep.wait()
    exchange_end(*ends)

    half = sp % 2

    def prefix(i, x):
        ps[i] = x.astype(BF16)
        return D[half, i][0:1, :] * x + rb[i].astype(F32)

    lax.fori_loop(0, SPAN, prefix, jnp.zeros((16, 512), F32))
    exchange_start(*priors)
    keep = pltpu.make_async_copy(ps.at[sp], pb.at[sp // 2, sp % 2], ls.at[2])
    keep.start()
    shared(GATE[1])
    project(GATE[1])
    do_gate(1)

    row = lax.broadcasted_iota(jnp.int32, (128, 128), 0)
    col = lax.broadcasted_iota(jnp.int32, (128, 128), 1)
    causal = (col <= row) & (row // BLOCK == col // BLOCK)

    def within(i, carry):
        at = pl.ds(pl.multiple_of(i * 128, 128), 128)
        for g in range(4):
            scores = jnp.where(causal, dot(R[g, at, :], IT[g, :, at]), 0.0).astype(BF16)
            B[g, at, :] = dot(scores, VB[g, at, :])
        return carry

    lax.fori_loop(0, 4, within, 0)
    cube_end(WAVES[2])
    keep.wait()
    exchange_end(*priors)
    for g in range(4):
        lane = (g % 2) * 256
        x = pb[:, g // 2, :, lane : lane + 256].reshape(128, 256).astype(F32)
        for b in range(8):
            em = EM[b, 0:1, g * 256 : g * 256 + 256]
            EN[g, b] = (em * x).astype(BF16)
            x = em * (em * x + ST[g, b])

    def finish(i, carry):
        at = pl.ds(pl.multiple_of(i * 128, 128), 128)
        squares = jnp.zeros((128, 1), F32)
        for g in range(4):
            r = R[g, at, :]
            across = jnp.concatenate(
                [dot(r[:BLOCK], EN[g, 2 * i]), dot(r[BLOCK:], EN[g, 2 * i + 1])], axis=0
            )
            mixed = A[g, at, :] * (B[g, at, :] + across)
            gated = rounded(mixed) * SG[g, at, :]
            GT[g] = gated
            squares = squares + jnp.sum(gated * gated, axis=1, keepdims=True)
        scale = lax.rsqrt(squares / WIDTH + 1.0)
        for g in range(4):
            lane = g * 256
            NORM[at, lane : lane + 256] = (GT[g] * scale * gain[:, lane : lane + 256]).astype(BF16)
        return carry

    lax.fori_loop(0, 4, finish, 0)
    cube_shared(WAVES[2])

    def project_out(n, carry):
        w = jnp.concatenate(
            [W[OUT[q // 2], q % 2, n].reshape(512, 256) for q in range(4)], axis=1
        )
        tile = lax.dot_general(
            NORM[...], w, (((1,), (1,)), ((), ())), preferred_element_type=F32
        )
        out[:, pl.ds(pl.multiple_of(n * 512, 512), 512)] = tile.astype(BF16)
        return carry

    lax.fori_loop(0, 4, project_out, 0)

    for started in pending:
        started.wait_send()
    for q in (totals, ends, priors):
        exchange_sent(*q)


def per_device(
    activations,
    value_weight,
    gate_weight,
    input_weight,
    readout_weight,
    rate_weight,
    value_taps,
    input_taps,
    readout_taps,
    rate_bias,
    decay_log,
    norm_gain,
    out_weight,
):
    vmem = pl.BlockSpec(memory_space=pltpu.VMEM)
    result = pl.pallas_call(
        kernel,
        out_shape=jax.ShapeDtypeStruct((ROWS, 2048), BF16),
        in_specs=[pl.BlockSpec(memory_space=pltpu.HBM)] * 6 + [vmem] * 7,
        out_specs=vmem,
        scratch_shapes=[
            pltpu.VMEM((8, 2, 4, 4, 4, 2, 16, 256), BF16),
            pltpu.VMEM((8, 16, 512), BF16),
            pltpu.VMEM((HALO + ROWS, 2048), BF16),
            pltpu.VMEM((HALO + ROWS, 512), F32),
            pltpu.VMEM((ROWS, 16), F32),
            pltpu.VMEM((4, ROWS, 256), F32),
            pltpu.VMEM((4, ROWS, 256), F32),
            pltpu.VMEM((8, 8, WIDTH), F32),
            pltpu.VMEM((4, ROWS, 256), BF16),
            pltpu.VMEM((4, 128, ROWS), BF16),
            pltpu.VMEM((4, ROWS, 128), BF16),
            pltpu.VMEM((4, ROWS, 256), F32),
            pltpu.VMEM((4, 8, 128, 256), F32),
            pltpu.VMEM((4, 8, 128, 256), BF16),
            pltpu.VMEM((8, 128), F32),
            pltpu.VMEM((SPAN, 8, 128), F32),
            pltpu.VMEM((2, SPAN, 8, 512), F32),
            pltpu.VMEM((8, 2, 16, 512), BF16),
            pltpu.VMEM((SPAN, 16, 512), BF16),
            pltpu.VMEM((SPAN, 16, 512), BF16),
            pltpu.VMEM((8, 2, 16, 512), BF16),
            pltpu.VMEM((4, 128, 256), F32),
            pltpu.VMEM((ROWS, WIDTH), BF16),
            pltpu.SemaphoreType.DMA((148,)),
            pltpu.SemaphoreType.DMA((148,)),
            pltpu.SemaphoreType.DMA((3, SPAN)),
            pltpu.SemaphoreType.DMA((3, SPAN)),
            pltpu.SemaphoreType.DMA((11,)),
            pltpu.SemaphoreType.REGULAR,
        ],
        compiler_params=pltpu.CompilerParams(
            collective_id=0, has_side_effects=True, vmem_limit_bytes=58 * 2**20
        ),
        name="mixer",
    )(
        activations[0],
        value_weight,
        gate_weight,
        input_weight,
        readout_weight,
        out_weight.T,
        rate_weight.T,
        value_taps,
        input_taps,
        readout_taps,
        rate_bias[None],
        decay_log[None],
        norm_gain[None],
    )
    return result[None]


def solution(mesh):
    placed = (
        P("dp", "sp", None),
        P(("sp", "dp"), None),
        P(("sp", "dp"), None),
        P(("sp", "dp"), None),
        P(("sp", "dp"), None),
        P(),
        P(),
        P(),
        P(),
        P(),
        P(),
        P(),
        P(None, ("sp", "dp")),
    )
    return jax.shard_map(
        per_device, mesh=mesh, in_specs=placed, out_specs=P("dp", "sp", None), check_vma=False
    )
```

```python
import jax
import jax.numpy as jnp
from jax import lax
from jax.experimental import pallas as pl
from jax.experimental.pallas import tpu as pltpu
from jax.sharding import PartitionSpec as P

F32 = jnp.float32
BF16 = jnp.bfloat16
MESH = pl.DeviceIdType.MESH

ROWS = 512
HALO = 16
LENGTH = 8192
WIDTH = 1024
BLOCK = 64
SPAN = 16

ORDER = (("x", "y", "z"), ("z", "x", "y"), ("y", "z", "x"))
STREAMS = ((0, 3), (3, 3), (6, 2))
VALUES, INPUTS, READS, GATE, OUT = (0, 3), 6, 1, (4, 7), (2, 5)


def silu(v):
    return (0.5 * v) * (1.0 + jnp.tanh(0.5 * v))


def rounded(v):
    return v.astype(BF16).astype(F32)


def split3(x):
    hi = x.astype(BF16)
    rest = x - hi.astype(F32)
    mid = rest.astype(BF16)
    return hi, mid, (rest - mid.astype(F32)).astype(BF16)


def dot(a, b):
    return jnp.dot(a, b, preferred_element_type=F32)


def spread(x, m):
    return sum(dot(part, m) for part in split3(x))


def kernel(
    act_hbm,
    value_w,
    gate_w,
    input_w,
    read_w,
    out_w,
    rate_w_hbm,
    value_taps_hbm,
    input_taps_hbm,
    read_taps_hbm,
    bias_hbm,
    decay_log_hbm,
    gain_hbm,
    out,
    rate_w,
    value_taps,
    input_taps,
    read_taps,
    bias,
    decay_log,
    gain,
    W,
    wcat,
    act,
    proj,
    rate_s,
    A,
    B,
    EM,
    VB,
    IT,
    R,
    SG,
    ST,
    EN,
    tb,
    tbuf,
    D,
    xs,
    rb,
    ps,
    pb,
    GT,
    NORM,
    ss,
    rs,
    ls,
    gs,
):
    sp = lax.axis_index("sp")
    dp = lax.axis_index("dp")
    c = {"z": sp // 4, "x": sp % 4, "y": dp // 2}
    core = dp % 2
    other = 1 - core
    partner = (sp, c["y"] * 2 + other)

    def neighbour(d, step, side=None):
        at = dict(c)
        at[d] = (c[d] + step) % 4
        return at["z"] * 4 + at["x"], at["y"] * 2 + (core if side is None else side)

    barrier = pltpu.get_barrier_semaphore()

    lines = [
        neighbour(d, step, side) for d in "xyz" for step in (1, 2, 3) for side in (core, other)
    ]
    for peer in lines + [partner]:
        pl.semaphore_signal(barrier, inc=1, device_id=peer, device_id_type=MESH)

    small = (
        (rate_w_hbm, rate_w),
        (value_taps_hbm, value_taps),
        (input_taps_hbm, input_taps),
        (read_taps_hbm, read_taps),
        (bias_hbm, bias),
        (decay_log_hbm, decay_log),
        (gain_hbm, gain),
    )
    load_small = [
        pltpu.make_async_copy(src, dst, ls.at[4 + n]) for n, (src, dst) in enumerate(small)
    ]
    load_act = pltpu.make_async_copy(act_hbm, act.at[pl.ds(HALO, ROWS)], ls.at[0])
    here = (c["z"], c["x"], c["y"])
    shards = (
        (value_w, 0),
        (read_w, 0),
        (out_w, 0),
        (value_w, 512),
        (gate_w, 0),
        (out_w, 512),
        (input_w, 0),
        (gate_w, 512),
    )

    load_w = [
        pltpu.make_async_copy(ref.at[:, pl.ds(at, 512)], wcat.at[stream], ls.at[3])
        for stream, (ref, at) in enumerate(shards)
    ]
    for load in [*load_w, load_act, *load_small]:
        load.start()
    pltpu.make_async_copy(wcat, wcat, ls.at[3]).wait()
    pl.semaphore_wait(barrier, 19)
    for step in (1, 2, 3):
        pl.semaphore_signal(gs, inc=1, device_id=neighbour("x", step), device_id_type=MESH)

    sent = []

    def send(src, dst, units, k, device):
        pltpu.make_async_remote_copy(
            src_ref=src,
            dst_ref=dst,
            send_sem=ss.at[0],
            recv_sem=rs.at[k],
            device_id=device,
            device_id_type=MESH,
        ).start()
        sent.append(units)

    def landed(view, k):
        pltpu.make_async_remote_copy(
            src_ref=view,
            dst_ref=view,
            send_sem=ss.at[0],
            recv_sem=rs.at[k],
            device_id=partner,
            device_id_type=MESH,
        ).wait_recv()

    def line_start(wave):
        for t, step in enumerate((1, 3, 2)):
            for stream in WAVES[wave]:
                for side in range(2):
                    send(
                        wcat.at[stream, :, side * 256 : side * 256 + 256],
                        W.at[(stream, side, *here, core)],
                        1,
                        wave,
                        neighbour(ORDER[stream // 3][0], step, side),
                    )

    def line_end(wave):
        landed(W.at[0 : len(WAVES[wave]), core, 0, 0, 0:3], wave)

    def piece(phase, stream, index, half=None, side=None):
        dims = ORDER[stream // 3]
        at = dict(c)
        for d in dims[:phase]:
            at[d] = slice(None)
        at[dims[phase]] = index
        if half is not None:
            d = [d for d in "zxy" if d in dims[:phase]][0]
            at[d] = slice(2 * half, 2 * half + 2)
        return W.at[stream, core if side is None else side, at["z"], at["x"], at["y"]]

    def axis(phase, stream):
        d = ORDER[stream // 3][phase]
        return d, c[d]

    def ring_start(phase, stream, k, units, part):
        d, i = axis(phase, stream)
        for half, near, far in ((part, k, k + 1), (1 - part, k, k + 1)):
            ahead = 1 if half == part else 3
            own = piece(phase, stream, i, half)
            send(own, own, units, near if part == 0 else far, neighbour(d, ahead))

    def ring_pass(phase, stream, k, units):
        d, i = axis(phase, stream)
        for half, back, ahead in ((0, 3, 1), (1, 1, 3)):
            block = piece(phase, stream, (i + back) % 4, half)
            send(block, block, units, k, neighbour(d, ahead))

    def share(stream, step, half):
        block = piece(2, stream, (axis(2, stream)[1] + step) % 4, half)
        send(block, block, 16, 33 + stream, partner)

    def shared(stream):
        landed(W.at[stream, other], 33 + stream)

    def planes_start(wave):
        for part in range(2):
            for stream in WAVES[wave]:
                ring_start(1, stream, 3 + 2 * wave, 4, part)

    def planes_pass(wave):
        landed(W.at[0 : len(WAVES[wave]), core, 0, 0], 3 + 2 * wave)
        for stream in WAVES[wave]:
            ring_pass(1, stream, 4 + 2 * wave, 4)

    def planes_end(wave):
        landed(W.at[0 : len(WAVES[wave]), core, 0, 0:2], 4 + 2 * wave)

    def cube_start(wave, parts=(0, 1)):
        for part in parts:
            for stream in WAVES[wave]:
                ring_start(2, stream, 9 + 3 * stream, 16, part)
                share(stream, 0, part)

    def cube_pass(wave):
        for stream in WAVES[wave]:
            landed(W.at[stream, core, 0], 9 + 3 * stream)
            ring_pass(2, stream, 11 + 3 * stream, 16)
            share(stream, 3, 0)
            share(stream, 1, 1)

    def cube_rest(wave):
        for stream in WAVES[wave]:
            landed(W.at[stream, core, 0], 10 + 3 * stream)
            share(stream, 3, 1)
            share(stream, 1, 0)

    def cube_end(wave):
        for stream in WAVES[wave]:
            landed(W.at[stream, core, 0], 11 + 3 * stream)
            share(stream, 2, 0)
            share(stream, 2, 1)

    def cube_shared(wave):
        for stream in WAVES[wave]:
            shared(stream)

    WAVES = ((6, 0, 3), (1, 4, 7), (2, 5))
    EDGE, GIVEN = 41, 42

    def exchange_start(q, src, dst, slots):
        def body(d, carry):
            j = (sp + d) % SPAN
            pltpu.make_async_remote_copy(
                src_ref=src(j),
                dst_ref=dst(sp),
                send_sem=ss.at[1 + q],
                recv_sem=rs.at[43 + q],
                device_id=(j, dp),
                device_id_type=MESH,
            ).start()
            return carry

        lax.fori_loop(1, SPAN, body, 0)

    def exchange_all(q, slots):
        view = slots.at[0 : SPAN - 1]
        return pltpu.make_async_remote_copy(
            src_ref=view,
            dst_ref=view,
            send_sem=ss.at[1 + q],
            recv_sem=rs.at[43 + q],
            device_id=partner,
            device_id_type=MESH,
        )

    def exchange_end(q, src, dst, slots):
        exchange_all(q, slots).wait_recv()

    def exchange_sent(q, src, dst, slots):
        exchange_all(q, slots).wait_send()

    totals = (0, lambda j: tb, lambda i: tbuf.at[i], tbuf)
    ends = (1, lambda j: xs.at[j // 2, j % 2], lambda i: rb.at[i], rb)
    priors = (2, lambda j: ps.at[j], lambda i: pb.at[i // 2, i % 2], ps)

    line_start(0)
    send(
        wcat.at[:, :, pl.ds(pl.multiple_of(other * 256, 256), 256)],
        W.at[(slice(None), other, *here, core)],
        8,
        GIVEN,
        partner,
    )
    keep_w = pltpu.make_async_copy(
        wcat.at[:, :, pl.ds(pl.multiple_of(core * 256, 256), 256)],
        W.at[(slice(None), core, *here, core)],
        ls.at[1],
    )
    keep_w.start()
    line_start(1)
    keep_w.wait()
    landed(W.at[(slice(None), core, *here, other)], GIVEN)
    line_end(0)
    planes_start(0)
    line_start(2)
    line_end(1)
    planes_start(1)
    pl.semaphore_wait(gs, 3)
    send(
        act_hbm.at[pl.ds(ROWS - HALO, HALO)],
        act.at[pl.ds(0, HALO)],
        8,
        EDGE,
        ((sp + 1) % SPAN, dp),
    )

    heads = lax.broadcasted_iota(jnp.int32, (16, WIDTH), 0)
    lanes = lax.broadcasted_iota(jnp.int32, (16, WIDTH), 1)
    expand = jnp.where(heads == lanes // 64, 1.0, 0.0).astype(BF16)
    load_act.wait()
    for load in load_small:
        load.wait()
    raw = lax.dot_general(
        act[HALO : HALO + ROWS, :],
        rate_w[...],
        (((1,), (1,)), ((), ())),
        preferred_element_type=F32,
    )
    raw = rounded(raw) + bias[...]
    rate_s[...] = jnp.maximum(raw, 0.0) + jnp.log1p(jnp.exp(-jnp.abs(raw)))

    tri_r = lax.broadcasted_iota(jnp.int32, (BLOCK, BLOCK), 0)
    tri_c = lax.broadcasted_iota(jnp.int32, (BLOCK, BLOCK), 1)
    tri = jnp.where(tri_c <= tri_r, 1.0, 0.0).astype(BF16)
    decay = -jnp.exp(decay_log[...]) / LENGTH

    def fading(b, total):
        at = pl.ds(pl.multiple_of(b * BLOCK, BLOCK), BLOCK)
        rate = rate_s[at, :]
        running = sum(dot(tri, part) for part in split3(rate * decay))
        end = running[BLOCK - 1 : BLOCK, :]
        mid = 0.5 * end
        a = spread(jnp.exp(running - mid), expand)
        bb = spread(jnp.exp(mid - running) * rate, expand)
        for g in range(4):
            A[g, at, :] = a[:, g * 256 : g * 256 + 256]
            B[g, at, :] = bb[:, g * 256 : g * 256 + 256]
        EM[b] = spread(jnp.broadcast_to(jnp.exp(mid), (8, 16)), expand)
        return total + end

    planes_pass(0)
    line_end(2)
    total = lax.fori_loop(0, 2, fading, jnp.zeros((1, 16), F32))
    planes_pass(1)
    planes_end(0)
    cube_start(0)
    planes_start(2)
    total = lax.fori_loop(2, 8, fading, total)
    eye = jnp.where(
        lax.broadcasted_iota(jnp.int32, (16, 128), 0)
        == lax.broadcasted_iota(jnp.int32, (16, 128), 1),
        1.0,
        0.0,
    ).astype(BF16)
    tb[...] = spread(jnp.broadcast_to(total, (8, 16)), eye)
    tbuf[sp] = tb[...]
    exchange_start(*totals)
    cube_pass(0)
    planes_end(1)
    cube_start(1)
    planes_pass(2)
    landed(act.at[pl.ds(0, HALO)], EDGE)

    @pl.when(sp == 0)
    def _():
        act[0:HALO, :] = jnp.zeros((HALO, 2048), BF16)

    cube_rest(0)
    cube_end(0)

    def project(stream):
        w = jnp.concatenate([W[stream, cc].reshape(2048, 256) for cc in range(2)], axis=1)
        proj[...] = rounded(dot(act[...], w))

    def convolved(at, lane, taps):
        rows = proj[pl.ds(pl.multiple_of(at + 8, 8), 136), lane : lane + 256]
        total = taps[3:4] * rows[8:136]
        for k in range(3):
            total = total + taps[k : k + 1] * rows[5 + k : 133 + k]
        return silu(total)

    def over_rows(body):
        def step(i, carry):
            body(pl.multiple_of(i * 128, 128))
            return carry

        lax.fori_loop(0, 4, step, 0)

    def do_values(which):
        lane = which * 512
        taps = value_taps[:, lane : lane + 512].astype(F32)

        def body(at):
            for cc in range(2):
                v = rounded(convolved(at, cc * 256, taps[:, cc * 256 : cc * 256 + 256]))
                g = 2 * which + cc
                VB[g, pl.ds(at, 128), :] = (v * B[g, pl.ds(at, 128), :]).astype(BF16)

        over_rows(body)

    def do_inputs():
        taps = input_taps[...].astype(F32)

        def body(at):
            for cc in range(2):
                v = convolved(at, cc * 256, taps[:, cc * 256 : cc * 256 + 256])
                for h in range(2):
                    part = v[:, h * 128 : h * 128 + 128]
                    IT[2 * cc + h, :, pl.ds(at, 128)] = part.T.astype(BF16)

        over_rows(body)

    def do_reads():
        taps = read_taps[...].astype(F32)

        def body(at):
            for cc in range(2):
                v = convolved(at, cc * 256, taps[:, cc * 256 : cc * 256 + 256]).astype(BF16)
                for h in range(2):
                    R[2 * cc + h, pl.ds(at, 128), :] = v[:, h * 128 : h * 128 + 128]

        over_rows(body)

    def do_gate(which):
        def body(at):
            for cc in range(2):
                SG[2 * which + cc, pl.ds(at, 128), :] = silu(
                    proj[pl.ds(at + HALO, 128), cc * 256 : cc * 256 + 256]
                )

        over_rows(body)

    shared(INPUTS)
    project(INPUTS)
    do_inputs()
    shared(VALUES[0])
    project(VALUES[0])
    cube_pass(1)
    planes_end(2)
    cube_start(2, (0,))
    do_values(0)
    shared(VALUES[1])
    project(VALUES[1])
    cube_rest(1)
    do_values(1)

    def block_states(i, carry):
        at = pl.ds(pl.multiple_of(i * 128, 128), 128)
        zero = jnp.zeros((BLOCK, 256), BF16)
        for g in range(4):
            v = VB[g, at, :]
            both = jnp.concatenate(
                [
                    jnp.concatenate([v[:BLOCK], zero], axis=0),
                    jnp.concatenate([zero, v[BLOCK:]], axis=0),
                ],
                axis=1,
            )
            states = dot(IT[g, :, at], both)
            ST[g, 2 * i] = states[:, :256]
            ST[g, 2 * i + 1] = states[:, 256:]
        return carry

    lax.fori_loop(0, 4, block_states, 0)
    for g in range(4):
        x = jnp.zeros((128, 256), F32)
        for b in range(8):
            em = EM[b, 0:1, g * 256 : g * 256 + 256]
            x = em * (em * x + ST[g, b])
        for n in range(8):
            xs[n, g // 2, :, (g % 2) * 256 : (g % 2) * 256 + 256] = x[n * 16 : n * 16 + 16].astype(
                BF16
            )
    exchange_start(*ends)
    keep = pltpu.make_async_copy(xs.at[sp // 2, sp % 2], rb.at[sp], ls.at[2])
    keep.start()
    cube_start(2, (1,))
    cube_end(1)
    exchange_end(*totals)
    expand128 = jnp.where(
        lax.broadcasted_iota(jnp.int32, (128, WIDTH), 0)
        == lax.broadcasted_iota(jnp.int32, (128, WIDTH), 1) // 64,
        1.0,
        0.0,
    ).astype(BF16)
    factors = spread(jnp.exp(tbuf[...].reshape(128, 128)), expand128).reshape(SPAN, 8, WIDTH)
    D[0] = factors[:, :, :512]
    D[1] = factors[:, :, 512:]

    shared(READS)
    project(READS)
    cube_pass(2)
    do_reads()
    keep.wait()
    exchange_end(*ends)

    half = sp % 2

    def prefix(i, x):
        ps[i] = x.astype(BF16)
        return D[half, i][0:1, :] * x + rb[i].astype(F32)

    lax.fori_loop(0, SPAN, prefix, jnp.zeros((16, 512), F32))
    exchange_start(*priors)
    keep = pltpu.make_async_copy(ps.at[sp], pb.at[sp // 2, sp % 2], ls.at[2])
    keep.start()
    shared(GATE[0])
    project(GATE[0])
    do_gate(0)
    shared(GATE[1])
    project(GATE[1])
    do_gate(1)

    row = lax.broadcasted_iota(jnp.int32, (128, 128), 0)
    col = lax.broadcasted_iota(jnp.int32, (128, 128), 1)
    causal = (col <= row) & (row // BLOCK == col // BLOCK)

    def within(i, carry):
        at = pl.ds(pl.multiple_of(i * 128, 128), 128)
        for g in range(4):
            scores = jnp.where(causal, dot(R[g, at, :], IT[g, :, at]), 0.0).astype(BF16)
            B[g, at, :] = dot(scores, VB[g, at, :])
        return carry

    lax.fori_loop(0, 4, within, 0)
    cube_rest(2)
    cube_end(2)
    keep.wait()
    exchange_end(*priors)
    for g in range(4):
        lane = (g % 2) * 256
        x = pb[:, g // 2, :, lane : lane + 256].reshape(128, 256).astype(F32)
        for b in range(8):
            em = EM[b, 0:1, g * 256 : g * 256 + 256]
            EN[g, b] = (em * x).astype(BF16)
            x = em * (em * x + ST[g, b])

    def finish(i, carry):
        at = pl.ds(pl.multiple_of(i * 128, 128), 128)
        squares = jnp.zeros((128, 1), F32)
        for g in range(4):
            r = R[g, at, :]
            across = jnp.concatenate(
                [dot(r[:BLOCK], EN[g, 2 * i]), dot(r[BLOCK:], EN[g, 2 * i + 1])], axis=0
            )
            mixed = A[g, at, :] * (B[g, at, :] + across)
            gated = rounded(mixed) * SG[g, at, :]
            GT[g] = gated
            squares = squares + jnp.sum(gated * gated, axis=1, keepdims=True)
        scale = lax.rsqrt(squares / WIDTH + 1.0)
        for g in range(4):
            lane = g * 256
            NORM[at, lane : lane + 256] = (GT[g] * scale * gain[:, lane : lane + 256]).astype(BF16)
        return carry

    lax.fori_loop(0, 4, finish, 0)
    cube_shared(2)

    def project_out(n, carry):
        w = jnp.concatenate(
            [W[OUT[q // 2], q % 2, n].reshape(512, 256) for q in range(4)], axis=1
        )
        tile = lax.dot_general(
            NORM[...], w, (((1,), (1,)), ((), ())), preferred_element_type=F32
        )
        out[:, pl.ds(pl.multiple_of(n * 512, 512), 512)] = tile.astype(BF16)
        return carry

    lax.fori_loop(0, 4, project_out, 0)

    assert sum(sent) == 2048
    pltpu.make_async_remote_copy(
        src_ref=W,
        dst_ref=W,
        send_sem=ss.at[0],
        recv_sem=rs.at[0],
        device_id=partner,
        device_id_type=MESH,
    ).wait_send()
    for q in (totals, ends, priors):
        exchange_sent(*q)


def per_device(
    activations,
    value_weight,
    gate_weight,
    input_weight,
    readout_weight,
    rate_weight,
    value_taps,
    input_taps,
    readout_taps,
    rate_bias,
    decay_log,
    norm_gain,
    out_weight,
):
    hbm = pl.BlockSpec(memory_space=pltpu.HBM)
    result = pl.pallas_call(
        kernel,
        out_shape=pltpu.VMEM((ROWS, 2048), BF16),
        in_specs=[hbm] * 13,
        out_specs=pl.BlockSpec(memory_space=pltpu.VMEM),
        scratch_shapes=[
            pltpu.VMEM((16, 2048), BF16),
            pltpu.VMEM((4, 1024), BF16),
            pltpu.VMEM((4, 512), BF16),
            pltpu.VMEM((4, 512), BF16),
            pltpu.VMEM((1, 16), F32),
            pltpu.VMEM((1, 16), F32),
            pltpu.VMEM((1, WIDTH), F32),
            pltpu.VMEM((8, 2, 4, 4, 4, 2, 16, 256), BF16),
            pltpu.VMEM((8, 16, 512), BF16),
            pltpu.VMEM((HALO + ROWS, 2048), BF16),
            pltpu.VMEM((HALO + ROWS, 512), F32),
            pltpu.VMEM((ROWS, 16), F32),
            pltpu.VMEM((4, ROWS, 256), F32),
            pltpu.VMEM((4, ROWS, 256), F32),
            pltpu.VMEM((8, 8, WIDTH), F32),
            pltpu.VMEM((4, ROWS, 256), BF16),
            pltpu.VMEM((4, 128, ROWS), BF16),
            pltpu.VMEM((4, ROWS, 128), BF16),
            pltpu.VMEM((4, ROWS, 256), F32),
            pltpu.VMEM((4, 8, 128, 256), F32),
            pltpu.VMEM((4, 8, 128, 256), BF16),
            pltpu.VMEM((8, 128), F32),
            pltpu.VMEM((SPAN, 8, 128), F32),
            pltpu.VMEM((2, SPAN, 8, 512), F32),
            pltpu.VMEM((8, 2, 16, 512), BF16),
            pltpu.VMEM((SPAN, 16, 512), BF16),
            pltpu.VMEM((SPAN, 16, 512), BF16),
            pltpu.VMEM((8, 2, 16, 512), BF16),
            pltpu.VMEM((4, 128, 256), F32),
            pltpu.VMEM((ROWS, WIDTH), BF16),
            pltpu.SemaphoreType.DMA((4,)),
            pltpu.SemaphoreType.DMA((46,)),
            pltpu.SemaphoreType.DMA((11,)),
            pltpu.SemaphoreType.REGULAR,
        ],
        compiler_params=pltpu.CompilerParams(
            collective_id=0, has_side_effects=True, vmem_limit_bytes=58 * 2**20
        ),
        name="mixer",
    )(
        activations[0],
        value_weight,
        gate_weight,
        input_weight,
        readout_weight,
        out_weight.T,
        rate_weight.T,
        value_taps,
        input_taps,
        readout_taps,
        rate_bias[None],
        decay_log[None],
        norm_gain[None],
    )
    return result[None]


def solution(mesh):
    placed = (
        P("dp", "sp", None),
        P(("sp", "dp"), None),
        P(("sp", "dp"), None),
        P(("sp", "dp"), None),
        P(("sp", "dp"), None),
        P(),
        P(),
        P(),
        P(),
        P(),
        P(),
        P(),
        P(None, ("sp", "dp")),
    )
    return jax.shard_map(
        per_device, mesh=mesh, in_specs=placed, out_specs=P("dp", "sp", None), check_vma=False
    )
```
